32 devices in a mesh: grp: 2 (over x), ep: 16 (over z, y, core).
Axes of the slice: x: 2, y: 2, z: 4, core: 2. Of those that a mesh axis runs over, the one named last changes fastest.
Arguments:
- hidden: bfloat16 [224, 2048], P(('grp', 'ep')), parts along dimension 0, may hold values from -6 to 6
- state_in: float32 [224, 64, 4096], P(('grp', 'ep')), parts along dimension 0, may hold values from -4 to 4
- conv_state: bfloat16 [224, 3, 4608], P(('grp', 'ep')), parts along dimension 0, may hold values from -6 to 6
- expert_ids: int32 [224, 4], P(('grp', 'ep')), parts along dimension 0, may hold values from 0 to 15, as said below
- group_prob: float32 [224], P(('grp', 'ep')), parts along dimension 0, may hold values from 0.25 to 1
- expert_score: float32 [224, 4], P(('grp', 'ep')), parts along dimension 0, may hold values from 0.05 to 1
- first_gain: bfloat16 [2048], replicated, may hold values from 0.099609375 to 1.8984375
- z_weight: bfloat16 [2048, 4096], P(None, 'ep'), may hold values from -0.125 to 0.125
- x_weight: bfloat16 [2048, 4096], P(None, 'ep'), may hold values from -0.125 to 0.125
- b_weight: bfloat16 [2048, 256], replicated, may hold values from -0.125 to 0.125
- c_weight: bfloat16 [2048, 256], replicated, may hold values from -0.125 to 0.125
- dt_weight: bfloat16 [2048, 64], replicated, may hold values from -0.125 to 0.125
- conv_weight: bfloat16 [4, 4608], replicated, may hold values from -3 to 3
- conv_bias: bfloat16 [4608], replicated, may hold values from -3 to 3
- dt_bias: float32 [64], replicated, may hold values from -4 to 0
- decay_log: float32 [64], replicated, may hold values from 0 to 2
- skip_gain: float32 [64], replicated, may hold values from 0.1 to 1.9
- inner_gain: bfloat16 [4096], replicated, may hold values from 0.099609375 to 1.8984375
- out_weight: bfloat16 [4096, 2048], P(None, 'ep'), may hold values from -0.09375 to 0.09375
- second_gain: bfloat16 [2048], replicated, may hold values from 0.099609375 to 1.8984375
- expert_gate: bfloat16 [16, 2048, 512], P('ep'), may hold values from -0.125 to 0.125
- expert_up: bfloat16 [16, 2048, 512], P('ep'), may hold values from -0.125 to 0.125
- expert_down: bfloat16 [16, 512, 2048], P('ep'), may hold values from -0.25 to 0.25
Outputs:
- layer_out: bfloat16 [224, 2048], P(('grp', 'ep')), parts along dimension 0
- state_out: float32 [224, 64, 4096], P(('grp', 'ep')), parts along dimension 0
- conv_out: bfloat16 [224, 3, 4608], P(('grp', 'ep')), parts along dimension 0
The draws below stay inside these ranges and needn't reach their ends.
There are 2 independent parts, one for each index of `grp`. The reference program is written for one: setup_inputs(seed, part) draws one part's arguments, and reference() takes and returns one part's arrays. A program takes and returns all parts, laid end to end along the dimension named above; an argument that names none is the same for every part. Nothing has to cross between parts.
Inputs may be any that keep to these rules, and one draw needn't show every extreme that they name: `expert_ids`: each row names 4 different experts of one expert group (numbers g * 8 to g * 8 + 7). Among the 7 rows of one device no expert is named more than 3 times, and in every draw one expert is named exactly 3 times by the rows of every device.
All inputs are finite; a program needn't handle non-finite values.
Results may differ from the reference program's by a relative error of at most 0.014.
Values may be sent and summed in bfloat16 or wider, within the bound.
A program may use at most 128 MiB of HBM per device.

```python
import math
import jax
import jax.numpy as jnp
from jax import lax

D = 2048
HEADS = 64
HEAD_DIM = 64
SSM_GROUPS = 4
STATE = 64
CONV = 4
MOE_HIDDEN = 512
EXP_GROUP = 8
TOP = 4
SEQ_DEV = 7
INNER = 4096
CONV_DIM = 4608
EXPERTS = 16
TOKENS = 112
CAP = 3
N_EP = 16


def draw_expert_ids(key, part):
    group_count = N_EP // EXP_GROUP
    hot_rows = min(SEQ_DEV, CAP + CAP * (EXP_GROUP - TOP) // TOP)
    hot_key, rest_key = jax.random.split(jax.random.fold_in(key, 11))
    hot_expert = jax.random.randint(hot_key, (), 0, N_EP)
    hot_group = hot_expert // EXP_GROUP
    hot_local = hot_expert % EXP_GROUP
    row_index = jnp.arange(SEQ_DEV, dtype=jnp.int32)[:, None]
    pick_index = jnp.arange(TOP, dtype=jnp.int32)[None, :]

    def one_block(block_key):
        key_order, key_inner, key_hot, key_shuffle, key_within = jax.random.split(block_key, 5)
        group_order = jax.random.permutation(key_order, group_count)
        sort_keys = (group_order == hot_group).astype(jnp.int32) * group_count + jnp.arange(group_count, dtype=jnp.int32)
        other_groups = group_order[jnp.argsort(sort_keys)][:group_count - 1]
        inner_keys = jax.random.split(key_inner, group_count - 1)
        inner_perm = jax.vmap(lambda one_key: jax.random.permutation(one_key, EXP_GROUP))(inner_keys)
        hot_perm = jax.random.permutation(key_hot, EXP_GROUP - 1)
        early_place = jnp.where(pick_index == 0, 0, 1 + (row_index * (TOP - 1) + pick_index - 1) % (EXP_GROUP - 1))
        late_place = 1 + (CAP * (TOP - 1) + (row_index - CAP) * TOP + pick_index) % (EXP_GROUP - 1)
        hot_place = jnp.where(row_index < CAP, early_place, late_place)
        hot_local_pick = jnp.where(hot_place == 0, hot_local, (hot_local + 1 + hot_perm[jnp.maximum(hot_place - 1, 0)]) % EXP_GROUP)
        hot_pick = hot_group * EXP_GROUP + hot_local_pick
        cold_row = jnp.maximum(row_index - hot_rows, 0)
        cold_group = cold_row % (group_count - 1)
        cold_turn = cold_row // (group_count - 1)
        cold_place = (cold_turn * TOP + pick_index) % EXP_GROUP
        cold_pick = other_groups[cold_group] * EXP_GROUP + inner_perm[cold_group, cold_place]
        block_ids = jnp.where(row_index < hot_rows, hot_pick, cold_pick)
        shuffle = jax.random.permutation(key_shuffle, SEQ_DEV)
        block_ids = block_ids[shuffle]
        within_keys = jax.random.split(key_within, SEQ_DEV)
        within = jax.vmap(lambda one_key: jax.random.permutation(one_key, TOP))(within_keys)
        return jnp.take_along_axis(block_ids, within, axis=1)
    block_keys = jax.random.split(rest_key, N_EP)
    return jax.vmap(one_block)(block_keys).reshape(N_EP * SEQ_DEV, TOP).astype(jnp.int32)


def block_levels(key, extent, cuts, least, high):
    level = 1.0
    for dim, blocks in cuts:
        heights = jax.random.uniform(jax.random.fold_in(jax.random.fold_in(key, 6), dim), (blocks,), jnp.float32, least / len(cuts), high / len(cuts))
        level = level * jnp.repeat(jnp.exp(heights), extent[dim] // blocks).reshape((-1,) + (1,) * (len(extent) - 1 - dim))
    return level


def normal_values(own_key, shape, width, limit, pieces=(), kind=jnp.bfloat16):
    loudness = block_levels(own_key, shape, pieces, -0.22, 0.18) if pieces else 1.0
    result = jax.random.normal(own_key, shape, jnp.float32) * width * loudness
    return jnp.minimum(jnp.maximum(result, -limit), limit).astype(kind)


def setup_inputs(seed: int = 0, part: int = 0) -> dict:
    key_list = jax.random.split(jax.random.key(seed), 24)
    part_splits = jax.random.split(jax.random.fold_in(key_list[23], part), 24)
    return {
        "hidden": normal_values(part_splits[0], (TOKENS, D), 1.0, 6.0, ((0, 16),)),
        "state_in": normal_values(part_splits[1], (TOKENS, HEADS, HEAD_DIM * STATE), 0.3, 4.0, ((0, 16),), jnp.float32),
        "conv_state": normal_values(part_splits[2], (TOKENS, CONV - 1, CONV_DIM), 1.0, 6.0, ((0, 16),)),
        "expert_ids": draw_expert_ids(jax.random.fold_in(jax.random.fold_in(key_list[23], part), 71), part),
        "group_prob": jnp.clip(jnp.exp(math.log(1.0) - 1.3862944 * jax.random.uniform(part_splits[4], (TOKENS,), jnp.float32) ** block_levels(part_splits[4], (TOKENS,), ((0, 16),), -0.2, 0.2)), 0.25, 1.0),
        "expert_score": jnp.clip(jnp.exp(math.log(1.0) - 2.9957323 * jax.random.uniform(part_splits[5], (TOKENS, TOP), jnp.float32) ** block_levels(part_splits[5], (TOKENS, TOP), ((0, 16),), -0.2, 0.2)), 0.05, 1.0),
        "first_gain": jnp.clip(1.0 + 0.18 * jax.random.normal(key_list[6], (D,), jnp.float32), 0.099609375, 1.8984375).astype(jnp.bfloat16),
        "z_weight": normal_values(key_list[7], (D, INNER), D ** -0.5, 0.125, ((1, 16),)),
        "x_weight": normal_values(key_list[8], (D, INNER), D ** -0.5, 0.125, ((1, 16),)),
        "b_weight": normal_values(key_list[9], (D, SSM_GROUPS * STATE), D ** -0.5, 0.125),
        "c_weight": normal_values(key_list[10], (D, SSM_GROUPS * STATE), D ** -0.5, 0.125),
        "dt_weight": normal_values(key_list[11], (D, HEADS), D ** -0.5, 0.125),
        "conv_weight": normal_values(key_list[12], (CONV, CONV_DIM), 0.5, 3.0),
        "conv_bias": normal_values(key_list[13], (CONV_DIM,), 0.5, 3.0),
        "dt_bias": jnp.clip(jax.random.uniform(key_list[14], (HEADS,), jnp.float32, -4.0, 0.0), -4.0, 0.0),
        "decay_log": jnp.clip(jax.random.uniform(key_list[15], (HEADS,), jnp.float32, 0.0, 2.0), 0.0, 2.0),
        "skip_gain": jnp.clip(1.0 + 0.18 * jax.random.normal(key_list[16], (HEADS,), jnp.float32), 0.1, 1.9),
        "inner_gain": jnp.clip(1.0 + 0.18 * jax.random.normal(key_list[17], (INNER,), jnp.float32), 0.099609375, 1.8984375).astype(jnp.bfloat16),
        "out_weight": normal_values(key_list[18], (INNER, D), INNER ** -0.5, 0.09375, ((1, 16),)),
        "second_gain": jnp.clip(1.0 + 0.18 * jax.random.normal(key_list[19], (D,), jnp.float32), 0.099609375, 1.8984375).astype(jnp.bfloat16),
        "expert_gate": normal_values(key_list[20], (EXPERTS, D, MOE_HIDDEN), D ** -0.5, 0.125, ((0, 16),)),
        "expert_up": normal_values(key_list[21], (EXPERTS, D, MOE_HIDDEN), D ** -0.5, 0.125, ((0, 16),)),
        "expert_down": normal_values(key_list[22], (EXPERTS, MOE_HIDDEN, D), MOE_HIDDEN ** -0.5, 0.25, ((0, 16),)),
    }


EPS = 1e-06

def rms_scale(values, gain_vec):
    return values * lax.rsqrt(lax.optimization_barrier(jnp.mean(values * values, axis=-1, keepdims=True)) + EPS) * gain_vec.astype(jnp.float32)

def state_step(active, dt_raw, state_in, dt_bias, decay_log, skip_gain):
    row_count = active.shape[0]
    inner_width = HEADS * HEAD_DIM
    state_span = SSM_GROUPS * STATE
    per_group = HEADS // SSM_GROUPS
    x_heads = active[:, :inner_width].reshape(row_count, HEADS, HEAD_DIM)
    b_input = active[:, inner_width:inner_width + state_span].reshape(row_count, SSM_GROUPS, STATE)
    c_input = active[:, inner_width + state_span:].reshape(row_count, SSM_GROUPS, STATE)
    b_heads = jnp.repeat(b_input, per_group, axis=1)
    c_heads = jnp.repeat(c_input, per_group, axis=1)
    step_size = jax.nn.softplus(dt_raw.astype(jnp.float32) + dt_bias[None, :])
    decay_rate = jnp.exp(-step_size * jnp.exp(decay_log)[None, :])
    carried = state_in.reshape(row_count, HEADS, HEAD_DIM, STATE)
    carried = decay_rate[:, :, None, None] * carried + (step_size[:, :, None] * x_heads)[:, :, :, None] * b_heads[:, :, None, :]
    readout = jnp.einsum('bhpn,bhn->bhp', carried, c_heads, precision=lax.Precision.HIGHEST)
    readout = readout + skip_gain[None, :, None] * x_heads
    return (readout.reshape(row_count, inner_width), carried.reshape(row_count, HEADS, HEAD_DIM * STATE))

def reference(hidden, state_in, conv_state, expert_ids, group_prob, expert_score, first_gain, z_weight, x_weight, b_weight, c_weight, dt_weight, conv_weight, conv_bias, dt_bias, decay_log, skip_gain, inner_gain, out_weight, second_gain, expert_gate, expert_up, expert_down):
    row_count = hidden.shape[0]
    normed = rms_scale(hidden.astype(jnp.float32), first_gain).astype(jnp.bfloat16)
    gate_z = jnp.dot(normed, z_weight, preferred_element_type=jnp.float32).astype(jnp.bfloat16)
    x_part = jnp.dot(normed, x_weight, preferred_element_type=jnp.float32).astype(jnp.bfloat16)
    b_part = jnp.dot(normed, b_weight, preferred_element_type=jnp.float32).astype(jnp.bfloat16)
    c_part = jnp.dot(normed, c_weight, preferred_element_type=jnp.float32).astype(jnp.bfloat16)
    dt_raw = jnp.dot(normed, dt_weight, preferred_element_type=jnp.float32).astype(jnp.bfloat16)
    fresh_input = jnp.concatenate([x_part, b_part, c_part], axis=1)
    window = jnp.concatenate([conv_state, fresh_input[:, None, :]], axis=1)
    summed = lax.optimization_barrier(jnp.sum(window.astype(jnp.float32) * conv_weight.astype(jnp.float32)[None], axis=1))
    active = jax.nn.silu(summed + conv_bias.astype(jnp.float32)[None, :])
    readout, state_out = state_step(active, dt_raw, state_in, dt_bias, decay_log, skip_gain)
    gated = readout * jax.nn.silu(gate_z.astype(jnp.float32))
    y_mix = rms_scale(gated, inner_gain).astype(jnp.bfloat16)
    projected = jnp.dot(y_mix, out_weight, preferred_element_type=jnp.float32).astype(jnp.bfloat16)
    projected = lax.optimization_barrier(projected)
    mixed_rows = (hidden.astype(jnp.float32) + projected.astype(jnp.float32)).astype(jnp.bfloat16)
    normed2 = rms_scale(mixed_rows.astype(jnp.float32), second_gain).astype(jnp.bfloat16)
    route_share = group_prob[:, None] * expert_score / lax.optimization_barrier(jnp.sum(expert_score, axis=1, keepdims=True))
    flat_ids = expert_ids.reshape(-1).astype(jnp.int32)
    flat_share = route_share.reshape(-1)
    route_count = flat_ids.shape[0]
    flat_rows = jnp.repeat(jnp.arange(row_count, dtype=jnp.int32), TOP)
    max_rows = N_EP * CAP

    def per_expert(accum, expert):
        is_routed = (flat_ids == expert).astype(jnp.int32)
        sort_keys = (1 - is_routed) * route_count + jnp.arange(route_count, dtype=jnp.int32)
        chosen = jnp.argsort(sort_keys)[:max_rows].astype(jnp.int32)
        token_rows = flat_rows[chosen]
        picked = normed2[token_rows]
        gate_part = jnp.dot(picked, expert_gate[expert], preferred_element_type=jnp.float32)
        up_part = jnp.dot(picked, expert_up[expert], preferred_element_type=jnp.float32)
        hidden_act = (jax.nn.silu(gate_part) * up_part).astype(jnp.bfloat16)
        expert_out = jnp.dot(hidden_act, expert_down[expert], preferred_element_type=jnp.float32).astype(jnp.bfloat16)
        expert_out = lax.optimization_barrier(expert_out)
        weight_vec = flat_share[chosen] * is_routed[chosen].astype(jnp.float32)
        accum = accum.at[token_rows].add(weight_vec[:, None] * expert_out.astype(jnp.float32))
        return (accum, None)
    blank = jnp.zeros((row_count, hidden.shape[1]), jnp.float32)
    moe_sum, _ = lax.scan(per_expert, blank, jnp.arange(EXPERTS, dtype=jnp.int32))
    layer_out = (mixed_rows.astype(jnp.float32) + moe_sum).astype(jnp.bfloat16)
    return (layer_out, state_out, window[:, 1:, :])
```

```python
import functools

import jax
import jax.numpy as jnp
from jax import lax
from jax.experimental import pallas as pl
from jax.experimental.pallas import tpu as pltpu
from jax.sharding import PartitionSpec as P

HEADS = 64
HEAD_DIM = 64
SSM_GROUPS = 4
STATE = 64
TOP = 4
EPS = 1e-06
MESH = pl.DeviceIdType.MESH
F32 = jnp.float32
BF16 = jnp.bfloat16
ROWS = 8


def rms_scale(values, gain_vec):
    return (
        values
        * lax.rsqrt(jnp.mean(values * values, axis=-1, keepdims=True) + EPS)
        * gain_vec.astype(F32)
    )


def peer(index):
    return (lax.axis_index("grp"), index)


def enter(n):
    me = lax.axis_index("ep")
    barrier = pltpu.get_barrier_semaphore()

    for d in range(1, n):
        pl.semaphore_signal(
            barrier, inc=1, device_id=peer(lax.rem(me + d, n)), device_id_type=MESH
        )
    pl.semaphore_wait(barrier, n - 1)


def remote(src, dst, send_sem, recv_sem, index):
    return pltpu.make_async_remote_copy(
        src_ref=src,
        dst_ref=dst,
        send_sem=send_sem,
        recv_sem=recv_sem,
        device_id=peer(index),
        device_id_type=MESH,
    )


def gather_start(n, src, buf, send, recv):
    me = lax.axis_index("ep")
    copies = []
    for d in range(1, n // 4):
        copy = remote(src, buf.at[me], send.at[d - 1], recv.at[d - 1], lax.rem(me + 4 * d, n))
        copy.start()
        copies.append(copy)
    return copies


def gather_finish(n, src, buf, send, recv, copies):
    me = lax.axis_index("ep")
    outer = n // 4
    core = lax.rem(me, 2)
    mid = lax.rem(me // 2, 2)
    mate = me + 1 - 2 * core
    across = me + 2 - 4 * mid
    second, third, fourth = [], [], []
    base = outer - 1
    for d in range(outer):
        block = lax.rem(me + n - 4 * d, n)
        if d > 0:
            copies[d - 1].wait_recv()
        piece = src if d == 0 else buf.at[block]
        copy = remote(piece, buf.at[block], send.at[base + d], recv.at[base + d], across)
        copy.start()
        second.append(copy)
        copy = remote(
            piece, buf.at[block], send.at[base + outer + d], recv.at[base + outer + d], mate
        )
        copy.start()
        third.append(copy)
    for d in range(outer):
        block = lax.rem(across + n - 4 * d, n)
        second[d].wait_recv()
        slot = base + 2 * outer + d
        copy = remote(buf.at[block], buf.at[block], send.at[slot], recv.at[slot], mate)
        copy.start()
        fourth.append(copy)
    for copy in third + fourth:
        copy.wait_recv()
    for copy in copies + second + third + fourth:
        copy.wait_send()


def exchange(n, out_buf, in_buf, send, recv):
    me = lax.axis_index("ep")
    copies = []
    for d in range(1, n):
        to = lax.rem(me + d, n)
        copy = remote(out_buf.at[to], in_buf.at[me], send.at[d - 1], recv.at[d - 1], to)
        copy.start()
        copies.append(copy)
    in_buf[me] = out_buf[me]
    for copy in copies:
        copy.wait_recv()
    for copy in copies:
        copy.wait_send()


def project_kernel(
    n,
    hid_ref,
    gain_ref,
    z_any,
    x_any,
    b_any,
    c_any,
    dt_any,
    all_ref,
    z_ref,
    x_ref,
    bc_ref,
    dt_ref,
    hbuf,
    normed,
    zw,
    xw,
    bw,
    cw,
    dw,
    out_buf,
    in_buf,
    wsem,
    gs,
    gr,
    es,
    er,
):
    loads = [
        pltpu.make_async_copy(src, dst, wsem.at[i])
        for i, (src, dst) in enumerate(
            [(b_any, bw), (c_any, cw), (dt_any, dw), (z_any, zw), (x_any, xw)]
        )
    ]
    for load in loads:
        load.start()
    enter(n)
    me = lax.axis_index("ep")
    copies = gather_start(n, hid_ref, hbuf, gs, gr)
    hbuf[me] = hid_ref[...]
    gain = gain_ref[...]
    mine = rms_scale(hid_ref[...].astype(F32), gain).astype(BF16)
    for load in loads[:3]:
        load.wait()
    span = bw.shape[1]
    bc_ref[:, :span] = jnp.dot(mine, bw[...], preferred_element_type=F32).astype(BF16).astype(F32)
    bc_ref[:, span:] = jnp.dot(mine, cw[...], preferred_element_type=F32).astype(BF16).astype(F32)
    dt_ref[...] = jnp.dot(mine, dw[...], preferred_element_type=F32).astype(BF16).astype(F32)
    gather_finish(n, hid_ref, hbuf, gs, gr, copies)
    for j in range(0, n, 2):
        pair = jnp.concatenate([hbuf[j].astype(F32), hbuf[j + 1].astype(F32)], axis=0)
        all_ref[j * ROWS : (j + 2) * ROWS, :] = pair.astype(BF16)
        normed[j * ROWS : (j + 2) * ROWS, :] = rms_scale(pair, gain).astype(BF16)
    for load in loads[3:]:
        load.wait()
    cols = zw.shape[1]
    z_part = jnp.dot(normed[...], zw[...], preferred_element_type=F32)
    x_part = jnp.dot(normed[...], xw[...], preferred_element_type=F32)
    for j in range(n):
        out_buf[j, :, :cols] = z_part[j * ROWS : (j + 1) * ROWS].astype(BF16)
        out_buf[j, :, cols:] = x_part[j * ROWS : (j + 1) * ROWS].astype(BF16)
    exchange(n, out_buf, in_buf, es, er)
    for j in range(n):
        z_ref[:, j * cols : (j + 1) * cols] = in_buf[j, :, :cols].astype(F32)
        x_ref[:, j * cols : (j + 1) * cols] = in_buf[j, :, cols:].astype(F32)


def project(n, hid8, first_gain, z_weight, x_weight, b_weight, c_weight, dt_weight):
    width = hid8.shape[1]
    cols = z_weight.shape[1]
    inner = n * cols
    span = b_weight.shape[1]
    vm = pl.BlockSpec(memory_space=pltpu.VMEM)
    hbm = pl.BlockSpec(memory_space=pl.ANY)
    dma = pltpu.SemaphoreType.DMA
    return pl.pallas_call(
        functools.partial(project_kernel, n),
        out_shape=(
            jax.ShapeDtypeStruct((n * ROWS, width), BF16),
            jax.ShapeDtypeStruct((ROWS, inner), F32),
            jax.ShapeDtypeStruct((ROWS, inner), F32),
            jax.ShapeDtypeStruct((ROWS, 2 * span), F32),
            jax.ShapeDtypeStruct((ROWS, dt_weight.shape[1]), F32),
        ),
        in_specs=[vm, vm] + [hbm] * 5,
        out_specs=(vm,) * 5,
        scratch_shapes=[
            pltpu.VMEM((n, ROWS, width), BF16),
            pltpu.VMEM((n * ROWS, width), BF16),
            pltpu.VMEM(z_weight.shape, BF16),
            pltpu.VMEM(x_weight.shape, BF16),
            pltpu.VMEM(b_weight.shape, BF16),
            pltpu.VMEM(c_weight.shape, BF16),
            pltpu.VMEM(dt_weight.shape, BF16),
            pltpu.VMEM((n, ROWS, 2 * cols), BF16),
            pltpu.VMEM((n, ROWS, 2 * cols), BF16),
            dma((5,)),
            dma((n - 1,)),
            dma((n - 1,)),
            dma((n - 1,)),
            dma((n - 1,)),
        ],
        compiler_params=pltpu.CompilerParams(
            collective_id=0, has_side_effects=True, vmem_limit_bytes=40 << 20
        ),
        name="project",
    )(hid8, first_gain[None, :], z_weight, x_weight, b_weight, c_weight, dt_weight)


def state_kernel(heads_ref, bc_ref, par_ref, gain_ref, st_ref, out_ref, y_ref):
    s = pl.program_id(0)
    heads = heads_ref[0]
    x = heads[:, :HEAD_DIM]
    z = heads[:, HEAD_DIM : 2 * HEAD_DIM]
    dt = heads[:, 2 * HEAD_DIM : 2 * HEAD_DIM + 1]
    par = par_ref[...]
    step = jax.nn.softplus(dt + par[:, 0:1])
    decay = jnp.exp(-step * jnp.exp(par[:, 1:2]))
    sx = step * x
    sx = jnp.concatenate([sx, sx], axis=1)
    row = bc_ref[pl.ds(s, 1), :]
    span = SSM_GROUPS * STATE
    per = HEADS // SSM_GROUPS
    bs, cs = [], []
    for g in range(SSM_GROUPS):
        b = row[:, g * STATE : (g + 1) * STATE]
        c = row[:, span + g * STATE : span + (g + 1) * STATE]
        bs.append(jnp.broadcast_to(jnp.concatenate([b, b], axis=1), (per, 2 * STATE)))
        cs.append(jnp.broadcast_to(jnp.concatenate([c, c], axis=1), (per, 2 * STATE)))
    b_all = jnp.concatenate(bs, axis=0)
    c_all = jnp.concatenate(cs, axis=0)
    decay = jnp.broadcast_to(decay, (HEADS, 128))
    half = lax.broadcasted_iota(jnp.int32, (HEADS, 128), 1) // STATE
    blocks = HEAD_DIM * STATE // 256
    k_of = lax.broadcasted_iota(jnp.int32, (256, 128), 0) // STATE
    l_of = lax.broadcasted_iota(jnp.int32, (256, 128), 1)
    fold = (k_of == l_of).astype(F32).astype(BF16)
    prods = []
    for k in range(blocks):
        parts = []
        for i in range(2):
            lane = (2 * k + i) * 128
            grown = jnp.take_along_axis(sx, half + (4 * k + 2 * i), axis=1)
            new = decay * st_ref[0, :, lane : lane + 128] + grown * b_all
            out_ref[0, :, lane : lane + 128] = new
            parts.append((new * c_all).astype(BF16))
        prods.append(jnp.concatenate(parts, axis=1))
    sums = jnp.dot(jnp.concatenate(prods, axis=0), fold, preferred_element_type=F32)
    total = sums[:HEADS]
    for k in range(1, blocks):
        total = total + pltpu.roll(sums[k * HEADS : (k + 1) * HEADS], 4 * k, 1)
    readout = total[:, :HEAD_DIM] + par[:, 2:3] * x
    gated = readout * jax.nn.silu(z)
    mean = jnp.sum(gated * gated, keepdims=True) / (HEADS * HEAD_DIM)
    y_ref[0] = gated * lax.rsqrt(mean + EPS) * gain_ref[...]


def state_update(heads, bc, par, gain, state_in):
    rows, _, flat = state_in.shape
    return pl.pallas_call(
        state_kernel,
        grid=(rows,),
        out_shape=(
            jax.ShapeDtypeStruct(state_in.shape, F32),
            jax.ShapeDtypeStruct((rows, HEADS, HEAD_DIM), F32),
        ),
        in_specs=[
            pl.BlockSpec((1,) + heads.shape[1:], lambda s: (s, 0, 0)),
            pl.BlockSpec(bc.shape, lambda s: (0, 0)),
            pl.BlockSpec(par.shape, lambda s: (0, 0)),
            pl.BlockSpec(gain.shape, lambda s: (0, 0)),
            pl.BlockSpec((1, HEADS, flat), lambda s: (s, 0, 0)),
        ],
        out_specs=(
            pl.BlockSpec((1, HEADS, flat), lambda s: (s, 0, 0)),
            pl.BlockSpec((1, HEADS, HEAD_DIM), lambda s: (s, 0, 0)),
        ),
        compiler_params=pltpu.CompilerParams(vmem_limit_bytes=40 << 20),
        name="state",
    )(heads, bc, par, gain, state_in)


def expert_kernel(
    n,
    cap,
    y_ref,
    hid_ref,
    own_ref,
    ids_ref,
    prob_ref,
    score_ref,
    gain_ref,
    ow_any,
    eg_any,
    eu_any,
    ed_any,
    out_ref,
    ybuf,
    yflat,
    pbuf,
    mixed,
    normed,
    act,
    eo,
    ow,
    eg,
    eu,
    ed,
    out_buf,
    in_buf,
    wsem,
    ys,
    yr,
    ps,
    pr,
    es,
    er,
):
    loads = [
        pltpu.make_async_copy(src, dst, wsem.at[i])
        for i, (src, dst) in enumerate(
            [(ow_any, ow), (eg_any.at[0], eg), (eu_any.at[0], eu), (ed_any.at[0], ed)]
        )
    ]
    for load in loads:
        load.start()
    enter(n)
    me = lax.axis_index("ep")
    total = n * ROWS
    copies = gather_start(n, y_ref, ybuf, ys, yr)
    ybuf[me] = y_ref[...]
    q = lax.broadcasted_iota(jnp.int32, (total, total), 0)
    t = lax.broadcasted_iota(jnp.int32, (total, total), 1)
    last = (t == (q // ROWS) * ROWS + (ROWS - 1)).astype(F32).astype(BF16)
    ids = jnp.dot(last, hid_ref[:, :128], preferred_element_type=F32)
    flags = (ids == me.astype(F32)).astype(F32).astype(BF16)
    lane = lax.broadcasted_iota(jnp.int32, (128, total), 0) // TOP
    token = lax.rem(lax.broadcasted_iota(jnp.int32, (128, total), 1), ROWS)
    here = jnp.dot(flags, (lane == token).astype(F32).astype(BF16), preferred_element_type=F32)
    before = jnp.dot(flags, (lane < token).astype(F32).astype(BF16), preferred_element_type=F32)
    slot = lax.rem(q, ROWS).astype(F32)
    chosen = (q // ROWS == t // ROWS) & (here > 0.5) & (before == slot)
    select = chosen.astype(F32).astype(BF16)
    rows = out_ref.shape[0]
    col = lax.broadcasted_iota(jnp.int32, (rows, n * cap), 1)
    score = score_ref[...]
    share = prob_ref[...] * score / jnp.sum(score, axis=1, keepdims=True)
    weight = jnp.zeros((rows, n * cap), F32)
    used = jnp.zeros((rows, n * cap), F32)
    for pick in range(TOP):
        hit = (ids_ref[:, pick : pick + 1] == col // cap).astype(F32)
        used = used + hit
        weight = weight + hit * share[:, pick : pick + 1]
    row_id = lax.broadcasted_iota(jnp.int32, (rows, n * cap), 0)
    rank = jnp.zeros((rows, n * cap), F32)
    for r in range(rows - 1):
        rank = rank + jnp.where(row_id > r, used[r : r + 1, :], 0.0)
    weight = jnp.where(rank == lax.rem(col, cap).astype(F32), weight, 0.0)
    high = weight.astype(BF16)
    low = (weight - high.astype(F32)).astype(BF16)
    gather_finish(n, y_ref, ybuf, ys, yr, copies)
    for j in range(0, n, 2):
        pair = jnp.concatenate([ybuf[j].astype(F32), ybuf[j + 1].astype(F32)], axis=0)
        yflat[j * ROWS : (j + 2) * ROWS, :] = pair.astype(BF16)
    loads[0].wait()
    pbuf[me] = jnp.dot(yflat[...], ow[...], preferred_element_type=F32).astype(BF16)
    copies = gather_start(n, pbuf.at[me], pbuf, ps, pr)
    gather_finish(n, pbuf.at[me], pbuf, ps, pr, copies)
    cols = pbuf.shape[2]
    for j in range(n):
        at = slice(j * cols, (j + 1) * cols)
        mixed[:, at] = (hid_ref[:, at].astype(F32) + pbuf[j].astype(F32)).astype(BF16)
    for j in range(0, total, 16):
        normed[j : j + 16, :] = rms_scale(mixed[j : j + 16, :].astype(F32), gain_ref[...]).astype(
            BF16
        )
    for load in loads[1:]:
        load.wait()
    for j in range(0, eg.shape[1], 256):
        at = slice(j, j + 256)
        gate = jnp.dot(normed[...], eg[:, at], preferred_element_type=F32)
        up = jnp.dot(normed[...], eu[:, at], preferred_element_type=F32)
        act[:, at] = (jax.nn.silu(gate) * up).astype(BF16)
    width = eo.shape[1]

    def down(i, carry):
        at = pl.ds(pl.multiple_of(i * 256, 256), 256)
        part = jnp.dot(act[...], ed[:, at], preferred_element_type=F32).astype(BF16)
        eo[:, at] = jnp.dot(select, part, preferred_element_type=F32)
        return carry

    lax.fori_loop(0, width // 256, down, 0)
    for j in range(n):
        out_buf[j] = eo[j * ROWS : j * ROWS + cap, :].astype(BF16)
    exchange(n, out_buf, in_buf, es, er)
    per = ROWS // cap
    for j in range(0, n, per):
        eo[j * cap : (j + per) * cap, :] = jnp.concatenate(
            [in_buf[j + i].astype(F32) for i in range(per)], axis=0
        )
    back = eo[: n * cap, :].astype(BF16)
    moe = jnp.dot(high, back, preferred_element_type=F32) + jnp.dot(
        low, back, preferred_element_type=F32
    )
    start = pl.multiple_of(me * ROWS, ROWS)
    eo[...] = mixed[...].astype(F32)
    out_ref[...] = (eo[pl.ds(start, ROWS), :][:rows] + moe).astype(BF16)


def experts(
    n, cap, y8, hid_all, hidden, ids, prob, score, second_gain, out_weight, gate_w, up_w, down_w
):
    total, width = hid_all.shape
    inner = y8.shape[1]
    cols = out_weight.shape[1]
    hid_units = gate_w.shape[2]
    vm = pl.BlockSpec(memory_space=pltpu.VMEM)
    hbm = pl.BlockSpec(memory_space=pl.ANY)
    dma = pltpu.SemaphoreType.DMA
    return pl.pallas_call(
        functools.partial(expert_kernel, n, cap),
        out_shape=jax.ShapeDtypeStruct(hidden.shape, BF16),
        in_specs=[vm] * 7 + [hbm] * 4,
        out_specs=vm,
        scratch_shapes=[
            pltpu.VMEM((n, ROWS, inner), BF16),
            pltpu.VMEM((total, inner), BF16),
            pltpu.VMEM((n, total, cols), BF16),
            pltpu.VMEM((total, width), BF16),
            pltpu.VMEM((total, width), BF16),
            pltpu.VMEM((total, hid_units), BF16),
            pltpu.VMEM((total, width), F32),
            pltpu.VMEM(out_weight.shape, BF16),
            pltpu.VMEM(gate_w.shape[1:], BF16),
            pltpu.VMEM(up_w.shape[1:], BF16),
            pltpu.VMEM(down_w.shape[1:], BF16),
            pltpu.VMEM((n, cap, width), BF16),
            pltpu.VMEM((n, cap, width), BF16),
            dma((4,)),
        ]
        + [dma((n - 1,))] * 6,
        compiler_params=pltpu.CompilerParams(
            collective_id=1, has_side_effects=True, vmem_limit_bytes=48 << 20
        ),
        name="experts",
    )(
        y8,
        hid_all,
        hidden,
        ids,
        prob[:, None],
        score,
        second_gain[None, :],
        out_weight,
        gate_w,
        up_w,
        down_w,
    )


def body(
    hidden,
    state_in,
    conv_state,
    expert_ids,
    group_prob,
    expert_score,
    first_gain,
    z_weight,
    x_weight,
    b_weight,
    c_weight,
    dt_weight,
    conv_weight,
    conv_bias,
    dt_bias,
    decay_log,
    skip_gain,
    inner_gain,
    out_weight,
    second_gain,
    expert_gate,
    expert_up,
    expert_down,
):
    n = lax.axis_size("ep")
    rows, width = hidden.shape
    inner = HEADS * HEAD_DIM
    id_row = jnp.pad(
        expert_ids.astype(BF16).reshape(1, -1),
        ((0, 0), (0, width - rows * TOP)),
        constant_values=-1,
    )
    hid8 = jnp.concatenate([hidden, id_row], axis=0)
    hid_all, z8, x8, bc8, dt8 = project(
        n, hid8, first_gain, z_weight, x_weight, b_weight, c_weight, dt_weight
    )
    fresh = jnp.concatenate([x8[:rows], bc8[:rows]], axis=1).astype(BF16)
    window = jnp.concatenate([conv_state, fresh[:, None, :]], axis=1)
    summed = jnp.sum(window.astype(F32) * conv_weight.astype(F32)[None], axis=1)
    active = jax.nn.silu(summed + conv_bias.astype(F32)[None, :])
    heads = jnp.concatenate(
        [
            active[:, :inner].reshape(rows, HEADS, HEAD_DIM),
            z8[:rows].reshape(rows, HEADS, HEAD_DIM),
            dt8[:rows][:, :, None],
        ],
        axis=2,
    )
    par = jnp.stack([dt_bias, decay_log, skip_gain], axis=1)
    state_out, y_heads = state_update(
        heads,
        active[:, inner:],
        par,
        inner_gain.astype(F32).reshape(HEADS, HEAD_DIM),
        state_in,
    )
    y8 = jnp.pad(y_heads.astype(BF16).reshape(rows, inner), ((0, ROWS - rows), (0, 0)))
    need = max(2, (3 * rows * TOP + 2 * n - 1) // (2 * n))
    cap = 2 if need <= 2 else 4 if need <= 4 else 8
    layer_out = experts(
        n,
        cap,
        y8,
        hid_all,
        hidden,
        expert_ids,
        group_prob,
        expert_score,
        second_gain,
        out_weight,
        expert_gate,
        expert_up,
        expert_down,
    )
    return (layer_out, state_out, window[:, 1:, :])


def solution(mesh):
    in_specs = (
        P(("grp", "ep"), None),
        P(("grp", "ep"), None, None),
        P(("grp", "ep"), None, None),
        P(("grp", "ep"), None),
        P(("grp", "ep")),
        P(("grp", "ep"), None),
        P(),
        P(None, "ep"),
        P(None, "ep"),
        P(),
        P(),
        P(),
        P(),
        P(),
        P(),
        P(),
        P(),
        P(),
        P(None, "ep"),
        P(),
        P("ep", None, None),
        P("ep", None, None),
        P("ep", None, None),
    )
    out_specs = (P(("grp", "ep"), None), P(("grp", "ep"), None, None), P(("grp", "ep"), None, None))
    return jax.shard_map(body, mesh=mesh, in_specs=in_specs, out_specs=out_specs, check_vma=False)
```

```python
import functools

import jax
import jax.numpy as jnp
from jax import lax
from jax.experimental import pallas as pl
from jax.experimental.pallas import tpu as pltpu
from jax.sharding import PartitionSpec as P

HEADS = 64
HEAD_DIM = 64
SSM_GROUPS = 4
STATE = 64
TOP = 4
EPS = 1e-06
MESH = pl.DeviceIdType.MESH
F32 = jnp.float32
BF16 = jnp.bfloat16
ROWS = 8


def rms_scale(values, gain_vec):
    return (
        values
        * lax.rsqrt(jnp.mean(values * values, axis=-1, keepdims=True) + EPS)
        * gain_vec.astype(F32)
    )


def peer(index):
    return (lax.axis_index("grp"), index)


def enter(n):
    me = lax.axis_index("ep")
    barrier = pltpu.get_barrier_semaphore()

    for d in range(1, n):
        pl.semaphore_signal(
            barrier, inc=1, device_id=peer(lax.rem(me + d, n)), device_id_type=MESH
        )
    pl.semaphore_wait(barrier, n - 1)


def remote(src, dst, send_sem, recv_sem, index):
    return pltpu.make_async_remote_copy(
        src_ref=src,
        dst_ref=dst,
        send_sem=send_sem,
        recv_sem=recv_sem,
        device_id=peer(index),
        device_id_type=MESH,
    )


def gather_start(n, src, buf, send, recv):
    me = lax.axis_index("ep")
    copies = []
    for d in range(1, n // 4):
        copy = remote(src, buf.at[me], send.at[d - 1], recv.at[d - 1], lax.rem(me + 4 * d, n))
        copy.start()
        copies.append(copy)
    return copies


def gather_finish(n, src, buf, send, recv, copies):
    me = lax.axis_index("ep")
    outer = n // 4
    core = lax.rem(me, 2)
    mid = lax.rem(me // 2, 2)
    mate = me + 1 - 2 * core
    across = me + 2 - 4 * mid
    second, third, fourth = [], [], []
    base = outer - 1
    for d in range(outer):
        block = lax.rem(me + n - 4 * d, n)
        if d > 0:
            copies[d - 1].wait_recv()
        piece = src if d == 0 else buf.at[block]
        copy = remote(piece, buf.at[block], send.at[base + d], recv.at[base + d], across)
        copy.start()
        second.append(copy)
        copy = remote(
            piece, buf.at[block], send.at[base + outer + d], recv.at[base + outer + d], mate
        )
        copy.start()
        third.append(copy)
    for d in range(outer):
        block = lax.rem(across + n - 4 * d, n)
        second[d].wait_recv()
        slot = base + 2 * outer + d
        copy = remote(buf.at[block], buf.at[block], send.at[slot], recv.at[slot], mate)
        copy.start()
        fourth.append(copy)
    for copy in third + fourth:
        copy.wait_recv()
    for copy in copies + second + third + fourth:
        copy.wait_send()


def exchange_start(n, out_buf, in_buf, send, recv):
    me = lax.axis_index("ep")
    copies = []
    for d in range(1, n):
        to = lax.rem(me + d, n)
        copy = remote(out_buf.at[to], in_buf.at[me], send.at[d - 1], recv.at[d - 1], to)
        copy.start()
        copies.append(copy)
    in_buf[me] = out_buf[me]
    return copies


def spread(ref):
    value = ref[...].astype(F32)
    return jnp.concatenate([value[i : i + 1] for i in range(value.shape[0])], axis=1)


def column(row):
    size = row.shape[1]
    at = lax.broadcasted_iota(jnp.int32, (size, size), 0)
    to = lax.broadcasted_iota(jnp.int32, (size, size), 1)
    return jnp.sum(jnp.where(at == to, row, jnp.zeros_like(row)), axis=1, keepdims=True)


def project_kernel(
    n,
    own_ref,
    ids_ref,
    gain_ref,
    z_any,
    x_any,
    b_any,
    c_any,
    dt_any,
    all_ref,
    z_ref,
    x_ref,
    bc_ref,
    dt_ref,
    hid_ref,
    hbuf,
    normed,
    zw,
    xw,
    bw,
    cw,
    dw,
    out_buf,
    in_buf,
    wsem,
    gs,
    gr,
    xs,
    xr,
    zs,
    zr,
):
    loads = [
        pltpu.make_async_copy(src, dst, wsem.at[i])
        for i, (src, dst) in enumerate(
            [(b_any, bw), (c_any, cw), (dt_any, dw), (z_any, zw), (x_any, xw)]
        )
    ]
    for load in loads:
        load.start()
    rows, width = own_ref.shape
    ids = ids_ref[...].astype(F32)
    pick = lax.broadcasted_iota(jnp.int32, (TOP, 128), 0)
    lane = lax.broadcasted_iota(jnp.int32, (TOP, 128), 1)
    spot = jnp.zeros((TOP, 128), F32)
    for r in range(rows):
        spot = spot + jnp.where(lane == TOP * r + pick, ids[:, r : r + 1] + 1.0, 0.0)
    id_row = jnp.sum(spot, axis=0, keepdims=True) - 1.0
    id_row = jnp.concatenate([id_row, jnp.full((1, width - 128), -1.0, F32)], axis=1)
    hid_ref[...] = jnp.concatenate([own_ref[...].astype(F32), id_row], axis=0).astype(BF16)
    enter(n)
    me = lax.axis_index("ep")
    copies = gather_start(n, hid_ref, hbuf, gs, gr)
    hbuf[me] = hid_ref[...]
    gain = spread(gain_ref)
    mine = rms_scale(hid_ref[...].astype(F32), gain).astype(BF16)
    for load in loads[:3]:
        load.wait()
    span = bw.shape[1]
    bc_ref[:, :span] = jnp.dot(mine, bw[...], preferred_element_type=F32).astype(BF16).astype(F32)
    bc_ref[:, span:] = jnp.dot(mine, cw[...], preferred_element_type=F32).astype(BF16).astype(F32)
    dt = lax.dot_general(mine, dw[...], (((1,), (1,)), ((), ())), preferred_element_type=F32)
    dt_ref[...] = dt.astype(BF16).astype(F32)
    gather_finish(n, hid_ref, hbuf, gs, gr, copies)
    for j in range(0, n, 2):
        pair = jnp.concatenate([hbuf[j].astype(F32), hbuf[j + 1].astype(F32)], axis=0)
        all_ref[j * ROWS : (j + 2) * ROWS, :] = pair.astype(BF16)
        normed[j * ROWS : (j + 2) * ROWS, :] = rms_scale(pair, gain).astype(BF16)
    for load in loads[3:]:
        load.wait()
    cols = zw.shape[1]
    flights = []
    for h, (weight, send, recv) in enumerate([(xw, xs, xr), (zw, zs, zr)]):
        part = jnp.dot(normed[...], weight[...], preferred_element_type=F32)
        for j in range(n):
            out_buf[h, j] = part[j * ROWS : (j + 1) * ROWS].astype(BF16)
        flights.append(exchange_start(n, out_buf.at[h], in_buf.at[h], send, recv))
    for h, ref in enumerate([x_ref, z_ref]):
        for copy in flights[h]:
            copy.wait_recv()
        for j in range(n):
            ref[:, j * cols : (j + 1) * cols] = in_buf[h, j].astype(F32)
    for copy in flights[0] + flights[1]:
        copy.wait_send()


def project(n, hidden, ids, first_gain, z_weight, x_weight, b_weight, c_weight, dt_weight):
    width = hidden.shape[1]
    cols = z_weight.shape[1]
    inner = n * cols
    span = b_weight.shape[1]
    vm = pl.BlockSpec(memory_space=pltpu.VMEM)
    hbm = pl.BlockSpec(memory_space=pl.ANY)
    dma = pltpu.SemaphoreType.DMA
    return pl.pallas_call(
        functools.partial(project_kernel, n),
        out_shape=(
            jax.ShapeDtypeStruct((n * ROWS, width), BF16),
            jax.ShapeDtypeStruct((ROWS, inner), F32),
            jax.ShapeDtypeStruct((ROWS, inner), F32),
            jax.ShapeDtypeStruct((ROWS, 2 * span), F32),
            jax.ShapeDtypeStruct((ROWS, dt_weight.shape[0]), F32),
        ),
        in_specs=[vm] * 3 + [hbm] * 5,
        out_specs=(vm,) * 5,
        scratch_shapes=[
            pltpu.VMEM((ROWS, width), BF16),
            pltpu.VMEM((n, ROWS, width), BF16),
            pltpu.VMEM((n * ROWS, width), BF16),
            pltpu.VMEM(z_weight.shape, BF16),
            pltpu.VMEM(x_weight.shape, BF16),
            pltpu.VMEM(b_weight.shape, BF16),
            pltpu.VMEM(c_weight.shape, BF16),
            pltpu.VMEM(dt_weight.shape, BF16),
            pltpu.VMEM((2, n, ROWS, cols), BF16),
            pltpu.VMEM((2, n, ROWS, cols), BF16),
            dma((5,)),
        ]
        + [dma((n - 1,))] * 6,
        compiler_params=pltpu.CompilerParams(
            collective_id=0, has_side_effects=True, vmem_limit_bytes=60 << 20
        ),
        name="project",
    )(hidden, ids.T, first_gain.reshape(-1, 128), z_weight, x_weight, b_weight, c_weight, dt_weight)


def state_kernel(heads_ref, bc_ref, par_ref, gain_ref, st_ref, out_ref, y_ref):
    s = pl.program_id(0)
    heads = heads_ref[0]
    x = heads[:, :HEAD_DIM]
    z = heads[:, HEAD_DIM : 2 * HEAD_DIM]
    dt = heads[:, 2 * HEAD_DIM : 2 * HEAD_DIM + 1]
    par = par_ref[...]
    step = jax.nn.softplus(dt + par[:, 0:1])
    decay = jnp.exp(-step * jnp.exp(par[:, 1:2]))
    sx = step * x
    sx = jnp.concatenate([sx, sx], axis=1)
    row = bc_ref[pl.ds(s, 1), :]
    span = SSM_GROUPS * STATE
    per = HEADS // SSM_GROUPS
    bs, cs = [], []
    for g in range(SSM_GROUPS):
        b = row[:, g * STATE : (g + 1) * STATE]
        c = row[:, span + g * STATE : span + (g + 1) * STATE]
        bs.append(jnp.broadcast_to(jnp.concatenate([b, b], axis=1), (per, 2 * STATE)))
        cs.append(jnp.broadcast_to(jnp.concatenate([c, c], axis=1), (per, 2 * STATE)))
    b_all = jnp.concatenate(bs, axis=0)
    c_all = jnp.concatenate(cs, axis=0)
    decay = jnp.broadcast_to(decay, (HEADS, 128))
    half = lax.broadcasted_iota(jnp.int32, (HEADS, 128), 1) // STATE
    blocks = HEAD_DIM * STATE // 256
    k_of = lax.broadcasted_iota(jnp.int32, (256, 128), 0) // STATE
    l_of = lax.broadcasted_iota(jnp.int32, (256, 128), 1)
    fold = (k_of == l_of).astype(F32).astype(BF16)
    prods = []
    for k in range(blocks):
        parts = []
        for i in range(2):
            lane = (2 * k + i) * 128
            grown = jnp.take_along_axis(sx, half + (4 * k + 2 * i), axis=1)
            new = decay * st_ref[0, :, lane : lane + 128] + grown * b_all
            out_ref[0, :, lane : lane + 128] = new
            parts.append((new * c_all).astype(BF16))
        prods.append(jnp.concatenate(parts, axis=1))
    sums = jnp.dot(jnp.concatenate(prods, axis=0), fold, preferred_element_type=F32)
    total = sums[:HEADS]
    for k in range(1, blocks):
        total = total + pltpu.roll(sums[k * HEADS : (k + 1) * HEADS], 4 * k, 1)
    readout = total[:, :HEAD_DIM] + par[:, 2:3] * x
    gated = readout * jax.nn.silu(z)
    mean = jnp.sum(gated * gated, keepdims=True) / (HEADS * HEAD_DIM)
    y_ref[0] = gated * lax.rsqrt(mean + EPS) * gain_ref[...]


def state_update(heads, bc, par, gain, state_in):
    rows, _, flat = state_in.shape
    return pl.pallas_call(
        state_kernel,
        grid=(rows,),
        out_shape=(
            jax.ShapeDtypeStruct(state_in.shape, F32),
            jax.ShapeDtypeStruct((rows, HEADS, HEAD_DIM), F32),
        ),
        in_specs=[
            pl.BlockSpec((1,) + heads.shape[1:], lambda s: (s, 0, 0)),
            pl.BlockSpec(bc.shape, lambda s: (0, 0)),
            pl.BlockSpec(par.shape, lambda s: (0, 0)),
            pl.BlockSpec(gain.shape, lambda s: (0, 0)),
            pl.BlockSpec((1, HEADS, flat), lambda s: (s, 0, 0)),
        ],
        out_specs=(
            pl.BlockSpec((1, HEADS, flat), lambda s: (s, 0, 0)),
            pl.BlockSpec((1, HEADS, HEAD_DIM), lambda s: (s, 0, 0)),
        ),
        compiler_params=pltpu.CompilerParams(vmem_limit_bytes=60 << 20),
        name="state",
    )(heads, bc, par, gain, state_in)


def expert_kernel(
    n,
    cap,
    y_ref,
    hid_ref,
    own_ref,
    ids_ref,
    prob_ref,
    score_ref,
    gain_ref,
    ow_any,
    eg_any,
    eu_any,
    ed_any,
    out_ref,
    ybuf,
    yflat,
    pbuf,
    mixed,
    normed,
    act,
    eo,
    ow,
    eg,
    eu,
    ed,
    out_buf,
    in_buf,
    wsem,
    ys,
    yr,
    ps,
    pr,
    es,
    er,
    fs,
    fr,
):
    loads = [
        pltpu.make_async_copy(src, dst, wsem.at[i])
        for i, (src, dst) in enumerate(
            [(ow_any, ow), (eg_any.at[0], eg), (eu_any.at[0], eu), (ed_any.at[0], ed)]
        )
    ]
    for load in loads:
        load.start()
    enter(n)
    me = lax.axis_index("ep")
    total = n * ROWS
    copies = gather_start(n, y_ref, ybuf, ys, yr)
    ybuf[me] = y_ref[...]
    q = lax.broadcasted_iota(jnp.int32, (total, total), 0)
    t = lax.broadcasted_iota(jnp.int32, (total, total), 1)
    last = (t == (q // ROWS) * ROWS + (ROWS - 1)).astype(F32).astype(BF16)
    ids = jnp.dot(last, hid_ref[:, :128], preferred_element_type=F32)
    flags = (ids == me.astype(F32)).astype(F32).astype(BF16)
    lane = lax.broadcasted_iota(jnp.int32, (128, total), 0) // TOP
    token = lax.rem(lax.broadcasted_iota(jnp.int32, (128, total), 1), ROWS)
    here = jnp.dot(flags, (lane == token).astype(F32).astype(BF16), preferred_element_type=F32)
    before = jnp.dot(flags, (lane < token).astype(F32).astype(BF16), preferred_element_type=F32)
    slot = lax.rem(q, ROWS).astype(F32)
    chosen = (q // ROWS == t // ROWS) & (here > 0.5) & (before == slot)
    select = chosen.astype(F32).astype(BF16)
    rows = out_ref.shape[0]
    col = lax.broadcasted_iota(jnp.int32, (rows, n * cap), 1)
    score = score_ref[...]
    share = prob_ref[...] * score / jnp.sum(score, axis=0, keepdims=True)
    ids = ids_ref[...].astype(F32)
    weight = jnp.zeros((rows, n * cap), F32)
    used = jnp.zeros((rows, n * cap), F32)
    for pick in range(TOP):
        hit = (column(ids[pick : pick + 1]) == (col // cap).astype(F32)).astype(F32)
        used = used + hit
        weight = weight + hit * column(share[pick : pick + 1])
    row_id = lax.broadcasted_iota(jnp.int32, (rows, n * cap), 0)
    rank = jnp.zeros((rows, n * cap), F32)
    for r in range(rows - 1):
        rank = rank + jnp.where(row_id > r, used[r : r + 1, :], 0.0)
    weight = jnp.where(rank == lax.rem(col, cap).astype(F32), weight, 0.0)
    high = weight.astype(BF16)
    low = (weight - high.astype(F32)).astype(BF16)
    gather_finish(n, y_ref, ybuf, ys, yr, copies)
    for j in range(0, n, 2):
        pair = jnp.concatenate([ybuf[j].astype(F32), ybuf[j + 1].astype(F32)], axis=0)
        yflat[j * ROWS : (j + 2) * ROWS, :] = pair.astype(BF16)
    loads[0].wait()
    pbuf[me] = jnp.dot(yflat[...], ow[...], preferred_element_type=F32).astype(BF16)
    copies = gather_start(n, pbuf.at[me], pbuf, ps, pr)
    gather_finish(n, pbuf.at[me], pbuf, ps, pr, copies)
    cols = pbuf.shape[2]
    for j in range(n):
        at = slice(j * cols, (j + 1) * cols)
        mixed[:, at] = (hid_ref[:, at].astype(F32) + pbuf[j].astype(F32)).astype(BF16)
    gain = spread(gain_ref)
    for j in range(0, total, 16):
        normed[j : j + 16, :] = rms_scale(mixed[j : j + 16, :].astype(F32), gain).astype(BF16)
    for load in loads[1:]:
        load.wait()
    for j in range(0, eg.shape[1], 256):
        at = slice(j, j + 256)
        gate = jnp.dot(normed[...], eg[:, at], preferred_element_type=F32)
        up = jnp.dot(normed[...], eu[:, at], preferred_element_type=F32)
        act[:, at] = (jax.nn.silu(gate) * up).astype(BF16)
    width = eo.shape[1]
    wide = width // 2
    tile = 256

    def down(i, carry):
        at = pl.ds(pl.multiple_of(i * tile, tile), tile)
        part = jnp.dot(act[...], ed[:, at], preferred_element_type=F32).astype(BF16)
        eo[:, at] = jnp.dot(select, part, preferred_element_type=F32)
        return carry

    flights = []
    for h, (send, recv) in enumerate([(es, er), (fs, fr)]):
        lax.fori_loop(h * wide // tile, (h + 1) * wide // tile, down, 0)
        for j in range(n):
            out_buf[h, j] = eo[j * ROWS : j * ROWS + cap, h * wide : (h + 1) * wide].astype(BF16)
        flights.append(exchange_start(n, out_buf.at[h], in_buf.at[h], send, recv))
    start = pl.multiple_of(me * ROWS, ROWS)
    eo[...] = mixed[...].astype(F32)
    base = eo[pl.ds(start, ROWS), :][:rows]
    per = ROWS // cap
    for h in range(2):
        for copy in flights[h]:
            copy.wait_recv()
        for j in range(0, n, per):
            eo[j * cap : (j + per) * cap, :wide] = jnp.concatenate(
                [in_buf[h, j + i].astype(F32) for i in range(per)], axis=0
            )
        back = eo[: n * cap, :wide].astype(BF16)
        moe = jnp.dot(high, back, preferred_element_type=F32) + jnp.dot(
            low, back, preferred_element_type=F32
        )
        at = slice(h * wide, (h + 1) * wide)
        out_ref[:, at] = (base[:, at] + moe).astype(BF16)
    for copy in flights[0] + flights[1]:
        copy.wait_send()


def experts(
    n, cap, y8, hid_all, hidden, ids, prob, score, second_gain, out_weight, gate_w, up_w, down_w
):
    total, width = hid_all.shape
    inner = y8.shape[1]
    cols = out_weight.shape[1]
    hid_units = gate_w.shape[2]
    vm = pl.BlockSpec(memory_space=pltpu.VMEM)
    hbm = pl.BlockSpec(memory_space=pl.ANY)
    dma = pltpu.SemaphoreType.DMA
    return pl.pallas_call(
        functools.partial(expert_kernel, n, cap),
        out_shape=jax.ShapeDtypeStruct(hidden.shape, BF16),
        in_specs=[vm] * 7 + [hbm] * 4,
        out_specs=vm,
        scratch_shapes=[
            pltpu.VMEM((n, ROWS, inner), BF16),
            pltpu.VMEM((total, inner), BF16),
            pltpu.VMEM((n, total, cols), BF16),
            pltpu.VMEM((total, width), BF16),
            pltpu.VMEM((total, width), BF16),
            pltpu.VMEM((total, hid_units), BF16),
            pltpu.VMEM((total, width), F32),
            pltpu.VMEM(out_weight.shape, BF16),
            pltpu.VMEM(gate_w.shape[1:], BF16),
            pltpu.VMEM(up_w.shape[1:], BF16),
            pltpu.VMEM(down_w.shape[1:], BF16),
            pltpu.VMEM((2, n, cap, width // 2), BF16),
            pltpu.VMEM((2, n, cap, width // 2), BF16),
            dma((4,)),
        ]
        + [dma((n - 1,))] * 8,
        compiler_params=pltpu.CompilerParams(
            collective_id=1, has_side_effects=True, vmem_limit_bytes=60 << 20
        ),
        name="experts",
    )(
        y8,
        hid_all,
        hidden,
        ids.T,
        prob[None, :],
        score.T,
        second_gain.reshape(-1, 128),
        out_weight,
        gate_w,
        up_w,
        down_w,
    )


def body(
    hidden,
    state_in,
    conv_state,
    expert_ids,
    group_prob,
    expert_score,
    first_gain,
    z_weight,
    x_weight,
    b_weight,
    c_weight,
    dt_weight,
    conv_weight,
    conv_bias,
    dt_bias,
    decay_log,
    skip_gain,
    inner_gain,
    out_weight,
    second_gain,
    expert_gate,
    expert_up,
    expert_down,
):
    n = lax.axis_size("ep")
    rows, width = hidden.shape
    inner = HEADS * HEAD_DIM
    hid_all, z8, x8, bc8, dt8 = project(
        n, hidden, expert_ids, first_gain, z_weight, x_weight, b_weight, c_weight, dt_weight.T
    )
    fresh = jnp.concatenate([x8[:rows], bc8[:rows]], axis=1).astype(BF16)
    taps = conv_weight.astype(F32)
    held = conv_state.shape[1]
    summed = jnp.sum(conv_state.astype(F32) * taps[None, :held], axis=1)
    summed = summed + fresh.astype(F32) * taps[held][None]
    conv_out = jnp.concatenate([conv_state[:, 1:], fresh[:, None, :]], axis=1)
    active = jax.nn.silu(summed + conv_bias.astype(F32)[None, :])
    heads = jnp.concatenate(
        [
            active[:, :inner].reshape(rows, HEADS, HEAD_DIM),
            z8[:rows].reshape(rows, HEADS, HEAD_DIM),
            dt8[:rows][:, :, None],
        ],
        axis=2,
    )
    par = jnp.stack([dt_bias, decay_log, skip_gain], axis=1)
    state_out, y_heads = state_update(
        heads,
        active[:, inner:],
        par,
        inner_gain.astype(F32).reshape(HEADS, HEAD_DIM),
        state_in,
    )
    y8 = jnp.pad(y_heads.astype(BF16).reshape(rows, inner), ((0, ROWS - rows), (0, 0)))
    need = max(2, (3 * rows * TOP + 2 * n - 1) // (2 * n))
    cap = 2 if need <= 2 else 4 if need <= 4 else 8
    layer_out = experts(
        n,
        cap,
        y8,
        hid_all,
        hidden,
        expert_ids,
        group_prob,
        expert_score,
        second_gain,
        out_weight,
        expert_gate,
        expert_up,
        expert_down,
    )
    return (layer_out, state_out, conv_out)


def solution(mesh):
    in_specs = (
        P(("grp", "ep"), None),
        P(("grp", "ep"), None, None),
        P(("grp", "ep"), None, None),
        P(("grp", "ep"), None),
        P(("grp", "ep")),
        P(("grp", "ep"), None),
        P(),
        P(None, "ep"),
        P(None, "ep"),
        P(),
        P(),
        P(),
        P(),
        P(),
        P(),
        P(),
        P(),
        P(),
        P(None, "ep"),
        P(),
        P("ep", None, None),
        P("ep", None, None),
        P("ep", None, None),
    )
    out_specs = (P(("grp", "ep"), None), P(("grp", "ep"), None, None), P(("grp", "ep"), None, None))
    return jax.shard_map(body, mesh=mesh, in_specs=in_specs, out_specs=out_specs, check_vma=False)
```

```python
import functools

import jax
import jax.numpy as jnp
from jax import lax
from jax.experimental import pallas as pl
from jax.experimental.pallas import tpu as pltpu
from jax.sharding import PartitionSpec as P

HEADS = 64
HEAD_DIM = 64
SSM_GROUPS = 4
STATE = 64
TOP = 4
EPS = 1e-06
MESH = pl.DeviceIdType.MESH
F32 = jnp.float32
BF16 = jnp.bfloat16
ROWS = 8


def rms_scale(values, gain_vec):
    return (
        values
        * lax.rsqrt(jnp.mean(values * values, axis=-1, keepdims=True) + EPS)
        * gain_vec.astype(F32)
    )


def peer(index):
    return (lax.axis_index("grp"), index)


def enter(n):
    me = lax.axis_index("ep")
    barrier = pltpu.get_barrier_semaphore()

    for d in range(1, n):
        pl.semaphore_signal(
            barrier, inc=1, device_id=peer(lax.rem(me + d, n)), device_id_type=MESH
        )
    pl.semaphore_wait(barrier, n - 1)


def remote(src, dst, send_sem, recv_sem, index):
    return pltpu.make_async_remote_copy(
        src_ref=src,
        dst_ref=dst,
        send_sem=send_sem,
        recv_sem=recv_sem,
        device_id=peer(index),
        device_id_type=MESH,
    )


def gather_start(n, src, buf, send, recv):
    me = lax.axis_index("ep")
    copies = []
    for d in range(1, n // 4):
        copy = remote(src, buf.at[me], send.at[d - 1], recv.at[d - 1], lax.rem(me + 4 * d, n))
        copy.start()
        copies.append(copy)
    return copies


def gather_finish(n, src, buf, send, recv, copies):
    me = lax.axis_index("ep")
    outer = n // 4
    core = lax.rem(me, 2)
    mid = lax.rem(me // 2, 2)
    mate = me + 1 - 2 * core
    across = me + 2 - 4 * mid
    second, third, fourth = [], [], []
    base = outer - 1
    for d in range(outer):
        block = lax.rem(me + n - 4 * d, n)
        if d > 0:
            copies[d - 1].wait_recv()
        piece = src if d == 0 else buf.at[block]
        copy = remote(piece, buf.at[block], send.at[base + d], recv.at[base + d], across)
        copy.start()
        second.append(copy)
        copy = remote(
            piece, buf.at[block], send.at[base + outer + d], recv.at[base + outer + d], mate
        )
        copy.start()
        third.append(copy)
    for d in range(outer):
        block = lax.rem(across + n - 4 * d, n)
        second[d].wait_recv()
        slot = base + 2 * outer + d
        copy = remote(buf.at[block], buf.at[block], send.at[slot], recv.at[slot], mate)
        copy.start()
        fourth.append(copy)
    for copy in third + fourth:
        copy.wait_recv()
    for copy in copies + second + third + fourth:
        copy.wait_send()


def exchange_start(n, out_buf, in_buf, send, recv):
    me = lax.axis_index("ep")
    copies = []
    for d in range(1, n):
        to = lax.rem(me + d, n)
        copy = remote(out_buf.at[to], in_buf.at[me], send.at[d - 1], recv.at[d - 1], to)
        copy.start()
        copies.append(copy)
    in_buf[me] = out_buf[me]
    return copies


def spread(ref):
    value = ref[...].astype(F32)
    return jnp.concatenate([value[i : i + 1] for i in range(value.shape[0])], axis=1)


def column(row):
    size = row.shape[1]
    at = lax.broadcasted_iota(jnp.int32, (size, size), 0)
    to = lax.broadcasted_iota(jnp.int32, (size, size), 1)
    return jnp.sum(jnp.where(at == to, row, jnp.zeros_like(row)), axis=1, keepdims=True)


def project_kernel(
    n,
    own_ref,
    ids_ref,
    gain_ref,
    z_any,
    x_any,
    b_any,
    c_any,
    dt_any,
    all_ref,
    z_ref,
    x_ref,
    bc_ref,
    dt_ref,
    hid_ref,
    hbuf,
    normed,
    zw,
    xw,
    bw,
    cw,
    dw,
    out_buf,
    in_buf,
    wsem,
    gs,
    gr,
    xs,
    xr,
    zs,
    zr,
):
    loads = [
        pltpu.make_async_copy(src, dst, wsem.at[i])
        for i, (src, dst) in enumerate(
            [(b_any, bw), (c_any, cw), (dt_any, dw), (z_any, zw), (x_any, xw)]
        )
    ]
    for load in loads:
        load.start()
    rows, width = own_ref.shape
    ids = ids_ref[...].astype(F32)
    pick = lax.broadcasted_iota(jnp.int32, (TOP, 128), 0)
    lane = lax.broadcasted_iota(jnp.int32, (TOP, 128), 1)
    spot = jnp.zeros((TOP, 128), F32)
    for r in range(rows):
        spot = spot + jnp.where(lane == TOP * r + pick, ids[:, r : r + 1] + 1.0, 0.0)
    id_row = jnp.sum(spot, axis=0, keepdims=True) - 1.0
    id_row = jnp.concatenate([id_row, jnp.full((1, width - 128), -1.0, F32)], axis=1)
    hid_ref[...] = jnp.concatenate([own_ref[...].astype(F32), id_row], axis=0).astype(BF16)
    enter(n)
    me = lax.axis_index("ep")
    copies = gather_start(n, hid_ref, hbuf, gs, gr)
    hbuf[me] = hid_ref[...]
    gain = spread(gain_ref)
    mine = rms_scale(hid_ref[...].astype(F32), gain).astype(BF16)
    for load in loads[:3]:
        load.wait()
    span = bw.shape[1]
    bc_ref[:, :span] = jnp.dot(mine, bw[...], preferred_element_type=F32).astype(BF16).astype(F32)
    bc_ref[:, span:] = jnp.dot(mine, cw[...], preferred_element_type=F32).astype(BF16).astype(F32)
    dt = lax.dot_general(mine, dw[...], (((1,), (1,)), ((), ())), preferred_element_type=F32)
    dt_ref[...] = dt.astype(BF16).astype(F32)
    gather_finish(n, hid_ref, hbuf, gs, gr, copies)
    for j in range(0, n, 2):
        pair = jnp.concatenate([hbuf[j].astype(F32), hbuf[j + 1].astype(F32)], axis=0)
        all_ref[j * ROWS : (j + 2) * ROWS, :] = pair.astype(BF16)
        normed[j * ROWS : (j + 2) * ROWS, :] = rms_scale(pair, gain).astype(BF16)
    for load in loads[3:]:
        load.wait()
    cols = zw.shape[1]
    flights = []
    for h, (weight, send, recv) in enumerate([(xw, xs, xr), (zw, zs, zr)]):
        part = jnp.dot(normed[...], weight[...], preferred_element_type=F32)
        for j in range(n):
            out_buf[h, j] = part[j * ROWS : (j + 1) * ROWS].astype(BF16)
        flights.append(exchange_start(n, out_buf.at[h], in_buf.at[h], send, recv))
    for h, ref in enumerate([x_ref, z_ref]):
        for copy in flights[h]:
            copy.wait_recv()
        for j in range(n):
            ref[:, j * cols : (j + 1) * cols] = in_buf[h, j].astype(F32)
    for copy in flights[0] + flights[1]:
        copy.wait_send()


def project(n, hidden, ids, first_gain, z_weight, x_weight, b_weight, c_weight, dt_weight):
    width = hidden.shape[1]
    cols = z_weight.shape[1]
    inner = n * cols
    span = b_weight.shape[1]
    vm = pl.BlockSpec(memory_space=pltpu.VMEM)
    hbm = pl.BlockSpec(memory_space=pl.ANY)
    dma = pltpu.SemaphoreType.DMA
    return pl.pallas_call(
        functools.partial(project_kernel, n),
        out_shape=(
            jax.ShapeDtypeStruct((n * ROWS, width), BF16),
            jax.ShapeDtypeStruct((ROWS, inner), F32),
            jax.ShapeDtypeStruct((ROWS, inner), F32),
            jax.ShapeDtypeStruct((ROWS, 2 * span), F32),
            jax.ShapeDtypeStruct((ROWS, dt_weight.shape[0]), F32),
        ),
        in_specs=[vm] * 3 + [hbm] * 5,
        out_specs=(vm,) * 5,
        scratch_shapes=[
            pltpu.VMEM((ROWS, width), BF16),
            pltpu.VMEM((n, ROWS, width), BF16),
            pltpu.VMEM((n * ROWS, width), BF16),
            pltpu.VMEM(z_weight.shape, BF16),
            pltpu.VMEM(x_weight.shape, BF16),
            pltpu.VMEM(b_weight.shape, BF16),
            pltpu.VMEM(c_weight.shape, BF16),
            pltpu.VMEM(dt_weight.shape, BF16),
            pltpu.VMEM((2, n, ROWS, cols), BF16),
            pltpu.VMEM((2, n, ROWS, cols), BF16),
            dma((5,)),
        ]
        + [dma((n - 1,))] * 6,
        compiler_params=pltpu.CompilerParams(
            collective_id=0, has_side_effects=True, vmem_limit_bytes=60 << 20
        ),
        name="project",
    )(hidden, ids.T, first_gain.reshape(-1, 128), z_weight, x_weight, b_weight, c_weight, dt_weight)


def state_kernel(heads_ref, bc_ref, par_ref, gain_ref, st_ref, out_ref, y_ref):
    s = pl.program_id(0)
    heads = heads_ref[0]
    x = heads[:, :HEAD_DIM]
    z = heads[:, HEAD_DIM : 2 * HEAD_DIM]
    dt = heads[:, 2 * HEAD_DIM : 2 * HEAD_DIM + 1]
    par = par_ref[...]
    step = jax.nn.softplus(dt + par[:, 0:1])
    decay = jnp.exp(-step * jnp.exp(par[:, 1:2]))
    sx = step * x
    sx = jnp.concatenate([sx, sx], axis=1)
    row = bc_ref[pl.ds(s, 1), :]
    span = SSM_GROUPS * STATE
    per = HEADS // SSM_GROUPS
    bs, cs = [], []
    for g in range(SSM_GROUPS):
        b = row[:, g * STATE : (g + 1) * STATE]
        c = row[:, span + g * STATE : span + (g + 1) * STATE]
        bs.append(jnp.broadcast_to(jnp.concatenate([b, b], axis=1), (per, 2 * STATE)))
        cs.append(jnp.broadcast_to(jnp.concatenate([c, c], axis=1), (per, 2 * STATE)))
    b_all = jnp.concatenate(bs, axis=0)
    c_all = jnp.concatenate(cs, axis=0)
    decay = jnp.broadcast_to(decay, (HEADS, 128))
    half = lax.broadcasted_iota(jnp.int32, (HEADS, 128), 1) // STATE
    blocks = HEAD_DIM * STATE // 256
    k_of = lax.broadcasted_iota(jnp.int32, (256, 128), 0) // STATE
    l_of = lax.broadcasted_iota(jnp.int32, (256, 128), 1)
    fold = (k_of == l_of).astype(F32).astype(BF16)
    prods = []
    for k in range(blocks):
        parts = []
        for i in range(2):
            lane = (2 * k + i) * 128
            grown = jnp.take_along_axis(sx, half + (4 * k + 2 * i), axis=1)
            new = decay * st_ref[0, :, lane : lane + 128] + grown * b_all
            out_ref[0, :, lane : lane + 128] = new
            parts.append((new * c_all).astype(BF16))
        prods.append(jnp.concatenate(parts, axis=1))
    sums = jnp.dot(jnp.concatenate(prods, axis=0), fold, preferred_element_type=F32)
    total = sums[:HEADS]
    for k in range(1, blocks):
        total = total + pltpu.roll(sums[k * HEADS : (k + 1) * HEADS], 4 * k, 1)
    readout = total[:, :HEAD_DIM] + par[:, 2:3] * x
    gated = readout * jax.nn.silu(z)
    mean = jnp.sum(gated * gated, keepdims=True) / (HEADS * HEAD_DIM)
    y_ref[0] = gated * lax.rsqrt(mean + EPS) * gain_ref[...]


def state_update(heads, bc, par, gain, state_in):
    rows, _, flat = state_in.shape
    return pl.pallas_call(
        state_kernel,
        grid=(rows,),
        out_shape=(
            jax.ShapeDtypeStruct(state_in.shape, F32),
            jax.ShapeDtypeStruct((rows, HEADS, HEAD_DIM), F32),
        ),
        in_specs=[
            pl.BlockSpec((1,) + heads.shape[1:], lambda s: (s, 0, 0)),
            pl.BlockSpec(bc.shape, lambda s: (0, 0)),
            pl.BlockSpec(par.shape, lambda s: (0, 0)),
            pl.BlockSpec(gain.shape, lambda s: (0, 0)),
            pl.BlockSpec((1, HEADS, flat), lambda s: (s, 0, 0)),
        ],
        out_specs=(
            pl.BlockSpec((1, HEADS, flat), lambda s: (s, 0, 0)),
            pl.BlockSpec((1, HEADS, HEAD_DIM), lambda s: (s, 0, 0)),
        ),
        compiler_params=pltpu.CompilerParams(vmem_limit_bytes=40 << 20),
        name="state",
    )(heads, bc, par, gain, state_in)


def expert_kernel(
    n,
    cap,
    y_ref,
    hid_ref,
    own_ref,
    ids_ref,
    prob_ref,
    score_ref,
    gain_ref,
    ow_any,
    eg_any,
    eu_any,
    ed_any,
    out_ref,
    ybuf,
    yflat,
    pbuf,
    mixed,
    normed,
    act,
    eo,
    ow,
    eg,
    eu,
    ed,
    out_buf,
    in_buf,
    wsem,
    ys,
    yr,
    ps,
    pr,
    es,
    er,
    fs,
    fr,
):
    loads = [
        pltpu.make_async_copy(src, dst, wsem.at[i])
        for i, (src, dst) in enumerate(
            [(ow_any, ow), (eg_any.at[0], eg), (eu_any.at[0], eu), (ed_any.at[0], ed)]
        )
    ]
    for load in loads:
        load.start()
    enter(n)
    me = lax.axis_index("ep")
    total = n * ROWS
    copies = gather_start(n, y_ref, ybuf, ys, yr)
    ybuf[me] = y_ref[...]
    q = lax.broadcasted_iota(jnp.int32, (total, total), 0)
    t = lax.broadcasted_iota(jnp.int32, (total, total), 1)
    last = (t == (q // ROWS) * ROWS + (ROWS - 1)).astype(F32).astype(BF16)
    ids = jnp.dot(last, hid_ref[:, :128], preferred_element_type=F32)
    flags = (ids == me.astype(F32)).astype(F32).astype(BF16)
    lane = lax.broadcasted_iota(jnp.int32, (128, total), 0) // TOP
    token = lax.rem(lax.broadcasted_iota(jnp.int32, (128, total), 1), ROWS)
    here = jnp.dot(flags, (lane == token).astype(F32).astype(BF16), preferred_element_type=F32)
    before = jnp.dot(flags, (lane < token).astype(F32).astype(BF16), preferred_element_type=F32)
    slot = lax.rem(q, ROWS).astype(F32)
    chosen = (q // ROWS == t // ROWS) & (here > 0.5) & (before == slot)
    select = chosen.astype(F32).astype(BF16)
    rows = out_ref.shape[0]
    col = lax.broadcasted_iota(jnp.int32, (rows, n * cap), 1)
    score = score_ref[...]
    share = prob_ref[...] * score / jnp.sum(score, axis=0, keepdims=True)
    ids = ids_ref[...].astype(F32)
    weight = jnp.zeros((rows, n * cap), F32)
    used = jnp.zeros((rows, n * cap), F32)
    for pick in range(TOP):
        hit = (column(ids[pick : pick + 1]) == (col // cap).astype(F32)).astype(F32)
        used = used + hit
        weight = weight + hit * column(share[pick : pick + 1])
    row_id = lax.broadcasted_iota(jnp.int32, (rows, n * cap), 0)
    rank = jnp.zeros((rows, n * cap), F32)
    for r in range(rows - 1):
        rank = rank + jnp.where(row_id > r, used[r : r + 1, :], 0.0)
    weight = jnp.where(rank == lax.rem(col, cap).astype(F32), weight, 0.0)
    high = weight.astype(BF16)
    low = (weight - high.astype(F32)).astype(BF16)
    gather_finish(n, y_ref, ybuf, ys, yr, copies)
    for j in range(0, n, 2):
        pair = jnp.concatenate([ybuf[j].astype(F32), ybuf[j + 1].astype(F32)], axis=0)
        yflat[j * ROWS : (j + 2) * ROWS, :] = pair.astype(BF16)
    loads[0].wait()
    pbuf[me] = jnp.dot(yflat[...], ow[...], preferred_element_type=F32).astype(BF16)
    copies = gather_start(n, pbuf.at[me], pbuf, ps, pr)
    gather_finish(n, pbuf.at[me], pbuf, ps, pr, copies)
    cols = pbuf.shape[2]
    for j in range(n):
        at = slice(j * cols, (j + 1) * cols)
        mixed[:, at] = (hid_ref[:, at].astype(F32) + pbuf[j].astype(F32)).astype(BF16)
    gain = spread(gain_ref)
    for j in range(0, total, 16):
        normed[j : j + 16, :] = rms_scale(mixed[j : j + 16, :].astype(F32), gain).astype(BF16)
    for load in loads[1:]:
        load.wait()
    for j in range(0, eg.shape[1], 256):
        at = slice(j, j + 256)
        gate = jnp.dot(normed[...], eg[:, at], preferred_element_type=F32)
        up = jnp.dot(normed[...], eu[:, at], preferred_element_type=F32)
        act[:, at] = (jax.nn.silu(gate) * up).astype(BF16)
    width = eo.shape[1]
    wide = width // 2
    tile = 256

    def down(i, carry):
        at = pl.ds(pl.multiple_of(i * tile, tile), tile)
        part = jnp.dot(act[...], ed[:, at], preferred_element_type=F32).astype(BF16)
        eo[:, at] = jnp.dot(select, part, preferred_element_type=F32)
        return carry

    flights = []
    for h, (send, recv) in enumerate([(es, er), (fs, fr)]):
        lax.fori_loop(h * wide // tile, (h + 1) * wide // tile, down, 0)
        for j in range(n):
            out_buf[h, j] = eo[j * ROWS : j * ROWS + cap, h * wide : (h + 1) * wide].astype(BF16)
        flights.append(exchange_start(n, out_buf.at[h], in_buf.at[h], send, recv))
    start = pl.multiple_of(me * ROWS, ROWS)
    eo[...] = mixed[...].astype(F32)
    base = eo[pl.ds(start, ROWS), :][:rows]
    per = ROWS // cap
    for h in range(2):
        for copy in flights[h]:
            copy.wait_recv()
        for j in range(0, n, per):
            eo[j * cap : (j + per) * cap, :wide] = jnp.concatenate(
                [in_buf[h, j + i].astype(F32) for i in range(per)], axis=0
            )
        back = eo[: n * cap, :wide].astype(BF16)
        moe = jnp.dot(high, back, preferred_element_type=F32) + jnp.dot(
            low, back, preferred_element_type=F32
        )
        at = slice(h * wide, (h + 1) * wide)
        out_ref[:, at] = (base[:, at] + moe).astype(BF16)
    for copy in flights[0] + flights[1]:
        copy.wait_send()


def experts(
    n, cap, y8, hid_all, hidden, ids, prob, score, second_gain, out_weight, gate_w, up_w, down_w
):
    total, width = hid_all.shape
    inner = y8.shape[1]
    cols = out_weight.shape[1]
    hid_units = gate_w.shape[2]
    vm = pl.BlockSpec(memory_space=pltpu.VMEM)
    hbm = pl.BlockSpec(memory_space=pl.ANY)
    dma = pltpu.SemaphoreType.DMA
    return pl.pallas_call(
        functools.partial(expert_kernel, n, cap),
        out_shape=jax.ShapeDtypeStruct(hidden.shape, BF16),
        in_specs=[vm] * 7 + [hbm] * 4,
        out_specs=vm,
        scratch_shapes=[
            pltpu.VMEM((n, ROWS, inner), BF16),
            pltpu.VMEM((total, inner), BF16),
            pltpu.VMEM((n, total, cols), BF16),
            pltpu.VMEM((total, width), BF16),
            pltpu.VMEM((total, width), BF16),
            pltpu.VMEM((total, hid_units), BF16),
            pltpu.VMEM((total, width), F32),
            pltpu.VMEM(out_weight.shape, BF16),
            pltpu.VMEM(gate_w.shape[1:], BF16),
            pltpu.VMEM(up_w.shape[1:], BF16),
            pltpu.VMEM(down_w.shape[1:], BF16),
            pltpu.VMEM((2, n, cap, width // 2), BF16),
            pltpu.VMEM((2, n, cap, width // 2), BF16),
            dma((4,)),
        ]
        + [dma((n - 1,))] * 8,
        compiler_params=pltpu.CompilerParams(
            collective_id=1, has_side_effects=True, vmem_limit_bytes=60 << 20
        ),
        name="experts",
    )(
        y8,
        hid_all,
        hidden,
        ids.T,
        prob[None, :],
        score.T,
        second_gain.reshape(-1, 128),
        out_weight,
        gate_w,
        up_w,
        down_w,
    )


def body(
    hidden,
    state_in,
    conv_state,
    expert_ids,
    group_prob,
    expert_score,
    first_gain,
    z_weight,
    x_weight,
    b_weight,
    c_weight,
    dt_weight,
    conv_weight,
    conv_bias,
    dt_bias,
    decay_log,
    skip_gain,
    inner_gain,
    out_weight,
    second_gain,
    expert_gate,
    expert_up,
    expert_down,
):
    n = lax.axis_size("ep")
    rows, width = hidden.shape
    inner = HEADS * HEAD_DIM
    hid_all, z8, x8, bc8, dt8 = project(
        n, hidden, expert_ids, first_gain, z_weight, x_weight, b_weight, c_weight, dt_weight.T
    )
    fresh = jnp.concatenate([x8[:rows], bc8[:rows]], axis=1).astype(BF16)
    taps = conv_weight.astype(F32)
    held = conv_state.shape[1]
    summed = jnp.sum(conv_state.astype(F32) * taps[None, :held], axis=1)
    summed = summed + fresh.astype(F32) * taps[held][None]
    conv_out = jnp.concatenate([conv_state[:, 1:], fresh[:, None, :]], axis=1)
    active = jax.nn.silu(summed + conv_bias.astype(F32)[None, :])
    heads = jnp.concatenate(
        [
            active[:, :inner].reshape(rows, HEADS, HEAD_DIM),
            z8[:rows].reshape(rows, HEADS, HEAD_DIM),
            dt8[:rows][:, :, None],
        ],
        axis=2,
    )
    par = jnp.stack([dt_bias, decay_log, skip_gain], axis=1)
    state_out, y_heads = state_update(
        heads,
        active[:, inner:],
        par,
        inner_gain.astype(F32).reshape(HEADS, HEAD_DIM),
        state_in,
    )
    y8 = jnp.pad(y_heads.astype(BF16).reshape(rows, inner), ((0, ROWS - rows), (0, 0)))
    need = max(2, (3 * rows * TOP + 2 * n - 1) // (2 * n))
    cap = 2 if need <= 2 else 4 if need <= 4 else 8
    layer_out = experts(
        n,
        cap,
        y8,
        hid_all,
        hidden,
        expert_ids,
        group_prob,
        expert_score,
        second_gain,
        out_weight,
        expert_gate,
        expert_up,
        expert_down,
    )
    return (layer_out, state_out, conv_out)


def solution(mesh):
    in_specs = (
        P(("grp", "ep"), None),
        P(("grp", "ep"), None, None),
        P(("grp", "ep"), None, None),
        P(("grp", "ep"), None),
        P(("grp", "ep")),
        P(("grp", "ep"), None),
        P(),
        P(None, "ep"),
        P(None, "ep"),
        P(),
        P(),
        P(),
        P(),
        P(),
        P(),
        P(),
        P(),
        P(),
        P(None, "ep"),
        P(),
        P("ep", None, None),
        P("ep", None, None),
        P("ep", None, None),
    )
    out_specs = (P(("grp", "ep"), None), P(("grp", "ep"), None, None), P(("grp", "ep"), None, None))
    return jax.shard_map(body, mesh=mesh, in_specs=in_specs, out_specs=out_specs, check_vma=False)
```
